32 devices in a mesh: ep: 8 (over z, x), tp: 4 (over y, core).
Axes of the slice: x: 2, y: 2, z: 4, core: 2. Of those that a mesh axis runs over, the one named last changes fastest.
Arguments:
- tokens: bfloat16 [128, 2048], P('ep'), may hold values from -6 to 6
- lengths: int32 [128], P('ep'), may hold values from 1 to 1024, as said below
- key_cache: bfloat16 [128, 1024, 8, 128], P('ep', None, 'tp'), may hold values from -200 to 200
- value_cache: bfloat16 [128, 1024, 8, 128], P('ep', None, 'tp'), may hold values from -6 to 6
- attn_gain: float32 [2048], replicated, may hold values from 0.1 to 1.9
- w_query: bfloat16 [2048, 8, 128], P(None, 'tp'), may hold values from -0.1875 to 0.1875
- w_key: bfloat16 [2048, 8, 128], P(None, 'tp'), may hold values from -0.15625 to 0.15625
- w_value: bfloat16 [2048, 8, 128], P(None, 'tp'), may hold values from -0.125 to 0.125
- mix_lambda: float32 [8], P('tp'), may hold values from 0.3 to 0.8
- head_gain: float32 [128], replicated, may hold values from 0.1 to 1.9
- w_out: bfloat16 [8, 128, 2048], P('tp'), may hold values from -2.5 to 2.5
- ffn_gain: float32 [2048], replicated, may hold values from 0.1 to 1.9
- w_gate: bfloat16 [8, 2048, 2048], P('ep', None, 'tp'), may hold values from -1 to 1
- w_up: bfloat16 [8, 2048, 2048], P('ep', None, 'tp'), may hold values from -1 to 1
- w_down: bfloat16 [8, 2048, 2048], P('ep', 'tp'), may hold values from -0.046875 to 0.046875
- routes: int32 [128, 4], P('ep'), may hold values from 0 to 7, all different within a row; in each aligned block of 16 rows (0 to 15, 16 to 31, ...) at most 16 rows name the same one
- route_weights: float32 [128, 4], P('ep'), may hold values from 0.1 to 1
Outputs:
- mixed: bfloat16 [128, 2048], P('ep', 'tp')
The draws below stay inside these ranges and needn't reach their ends.
Inputs may be any that keep to these rules, and one draw needn't show every extreme that they name: `routes`: in each aligned block of 16 rows no expert is named by more than 16 entries, and one is named by exactly 16 in some block; each row names 4 different experts. `lengths`: some sequence has all 1024 positions valid.
All inputs are finite; a program needn't handle non-finite values.
Results may differ from the reference program's by a relative error of at most 0.02.
The reference program's roundings to bfloat16 on the way count: a program that leaves them out, or rounds other values in their place, can miss the bound.
Values may be sent and summed in bfloat16 or wider, within the bound.
No kernel may reach another device: no remote copies, remote signals or barrier semaphores. Data moves between devices by JAX's collectives and lax.ppermute only.
A program may use at most 128 MiB of HBM per device.

```python
import math
import jax
import jax.numpy as jnp
import numpy as np
from jax import lax

D = 2048
HEADS = 8
HALF = 64
VDIM = 128
FF = 2048
TOP = 4
SEQ_DEV = 16
LEN = 1024
SEQS = 128
EXPERTS = 8
CAP = 16
GROUP_HEADS = 2
FF_DEV = 512
N_TP = 4


def draw_key_cache(key, part):
    base = jnp.clip(jax.random.normal(jax.random.fold_in(key, 11), (SEQS, LEN, HEADS, VDIM), jnp.float32), -6.0, 6.0)
    return base.astype(jnp.bfloat16)


def draw_lengths(key, part):
    groups = SEQS // SEQ_DEV
    limits = jax.random.randint(jax.random.fold_in(key, 21), (groups,), LEN // 8, LEN + 1)
    fullest = jax.random.randint(jax.random.fold_in(key, 22), (), 0, groups)
    group_ids = lax.iota(jnp.int32, groups)
    limits = jnp.where(group_ids == fullest, LEN, limits)
    raw_bits = jax.random.randint(jax.random.fold_in(key, 23), (groups, SEQ_DEV), 0, 1 << 30)
    seq_lengths = raw_bits % limits[:, None] + 1
    chosen_seq = jax.random.randint(jax.random.fold_in(key, 24), (), 0, SEQ_DEV)
    hit = (group_ids[:, None] == fullest) & (lax.iota(jnp.int32, SEQ_DEV)[None, :] == chosen_seq)
    seq_lengths = jnp.where(hit, LEN, seq_lengths)
    return seq_lengths.reshape(SEQS).astype(jnp.int32)


def shard_levels(own_key, shape, cuts, smallest, high):
    factor_of, own = 1.0, jax.random.fold_in(own_key, 6)
    for axis_at, shards_of in cuts:
        draws = jnp.exp(jax.random.uniform(jax.random.fold_in(own, axis_at), (shards_of,), jnp.float32, smallest / len(cuts), high / len(cuts)))
        factor_of = factor_of * jnp.repeat(draws, shape[axis_at] // shards_of).reshape([-1 if axis == axis_at else 1 for axis in range(len(shape))])
    return factor_of


def routed_block(stream_key, own, number, rows, count, top, bound, lean):
    order = jax.random.permutation(stream_key, count)
    heavy_load, usual = portions_of(count, rows * top, bound, lean, True), portions_of(count, rows * top, bound, lean, False)
    places = jnp.arange(count)

    def named(sizes, rotation):
        used = int((sizes > 0).sum())
        fixed = max(1, used // 4)
        moved = fixed + (places - fixed + rotation * (used - fixed)) % max(1, count - fixed)
        return jnp.zeros((count,), jnp.int32).at[order[jnp.where(places < fixed, places, moved)]].set(jnp.asarray(sizes, jnp.int32))

    sizes = jnp.where(number % 4 == 0, named(heavy_load, number // 4), named(usual, number - number // 4 - 1))
    mixed = jax.random.permutation(jax.random.fold_in(own, 3), count)
    source_of, receiver = mixed[0:count // 2 * 2:2], mixed[1:count // 2 * 2:2]
    room = jnp.minimum(sizes[source_of] - 1, bound - sizes[receiver]) // 2
    room = jnp.where((source_of == order[0]) | (receiver == order[0]) | (sizes[receiver] == 0), 0, jnp.maximum(room, 0))
    moved = jax.random.randint(jax.random.fold_in(own, 4), (count // 2,), 0, 1 << 20) % (room + 1)
    sizes = sizes.at[source_of].add(-moved).at[receiver].add(moved)
    members = jnp.searchsorted(jnp.cumsum(sizes), jnp.arange(rows * top), side="right").astype(jnp.int32)
    grid = members.reshape(top, rows).T
    grid = grid[jax.random.permutation(jax.random.fold_in(own, 1), rows)]
    rotation = jax.random.randint(jax.random.fold_in(own, 2), (rows, 1), 0, top)
    return jnp.take_along_axis(grid, (jnp.arange(top)[None, :] + rotation) % top, axis=1)


def portions_of(count, total, bound, slope, full):
    loads = [(1 << 20) // math.isqrt(rank ** slope) + 1 for rank in range(1, count + 1)]
    largest = bound if full else min(bound, max(-(-total // count), total * loads[0] // sum(loads)))
    least = 1 if total - largest >= count - 1 else 0
    holding, spare = [largest] + [least] * (count - 1), total - largest - least * (count - 1)
    while spare > 0:
        free = [i for i in range(1, count) if holding[i] < largest] or [i for i in range(1, count) if holding[i] < bound]
        pool, left = sum([loads[i] for i in free]), spare
        for i in free:
            more = min(bound - holding[i], max(1, left * loads[i] // pool), spare)
            holding[i] = holding[i] + more
            spare = spare - more
    return np.array(holding)


def centred(rng, shape, spread, most, cuts=(), dtype=jnp.bfloat16):
    loudness = shard_levels(rng, shape, cuts, -0.22, 0.18) if cuts else 1.0
    array = jax.random.normal(rng, shape, jnp.float32) * spread * loudness
    return jnp.minimum(jnp.maximum(array, -most), most).astype(dtype)


def setup_inputs(seed: int = 0) -> dict:
    key_of = jax.random.split(jax.random.key(seed), 18)
    tokens = centred(key_of[0], (SEQS, D), 1.0, 6.0, ((0, 8),))
    lengths = draw_lengths(jax.random.fold_in(key_of[17], 71), 0)
    key_cache = draw_key_cache(jax.random.fold_in(key_of[17], 71), 0)
    value_cache = centred(key_of[3], (SEQS, LEN, HEADS, VDIM), 1.0, 6.0, ((0, 8), (2, 4)))
    attn_gain = jnp.clip(1.0 + 0.18 * jax.random.normal(key_of[4], (D,), jnp.float32), 0.1, 1.9)
    w_query = centred(key_of[5], (D, HEADS, VDIM), (D // 2) ** -0.5, 0.1875, ((1, 4),))
    w_key = centred(key_of[6], (D, HEADS, VDIM), (D * 2 // 3) ** -0.5, 0.15625, ((1, 4),))
    w_value = centred(key_of[7], (D, HEADS, VDIM), D ** -0.5, 0.125, ((1, 4),))
    mix_lambda = jnp.clip(0.3 + 0.5 * jax.random.uniform(key_of[8], (HEADS,), jnp.float32) ** shard_levels(key_of[8], (HEADS,), ((0, 4),), -0.2, 0.2), 0.3, 0.8)
    head_gain = jnp.clip(1.0 + 0.18 * jax.random.normal(key_of[9], (VDIM,), jnp.float32), 0.1, 1.9)
    w_out = centred(key_of[10], (HEADS, VDIM, D), (5.0 / (HEADS * VDIM) ** 0.5), 2.5, ((0, 4),))
    ffn_gain = jnp.clip(1.0 + 0.18 * jax.random.normal(key_of[11], (D,), jnp.float32), 0.1, 1.9)
    w_gate = centred(key_of[12], (EXPERTS, D, FF), (3.0 / D ** 0.5), 1.0, ((0, 8), (2, 4)))
    w_up = centred(key_of[13], (EXPERTS, D, FF), (3.0 / D ** 0.5), 1.0, ((0, 8), (2, 4)))
    w_down = centred(key_of[14], (EXPERTS, FF, D), (0.15 / FF ** 0.5), 0.046875, ((0, 8), (1, 4)))
    routes_keys = jax.random.split(jax.random.fold_in(key_of[15], 1), SEQS // SEQ_DEV)
    routes_turns = jax.random.permutation(jax.random.fold_in(key_of[15], 3), SEQS // SEQ_DEV)
    routes = jax.vmap(lambda own, number: routed_block(jax.random.fold_in(key_of[15], 2), own, number, SEQ_DEV, EXPERTS, TOP, CAP, 2))(routes_keys, routes_turns).reshape((SEQS, TOP))
    route_weights = jnp.clip(0.1 + 0.9 * jax.random.uniform(key_of[16], (SEQS, TOP), jnp.float32) ** shard_levels(key_of[16], (SEQS, TOP), ((0, 8),), -0.2, 0.2), 0.1, 1.0)
    return dict(tokens=tokens, lengths=lengths, key_cache=key_cache, value_cache=value_cache, attn_gain=attn_gain, w_query=w_query, w_key=w_key, w_value=w_value, mix_lambda=mix_lambda, head_gain=head_gain, w_out=w_out, ffn_gain=ffn_gain, w_gate=w_gate, w_up=w_up, w_down=w_down, routes=routes, route_weights=route_weights)


epsilon = 1e-06
clamp_limit = 7.0
sigmoid_slope = 1.702
branch_scale = 0.2

def norm_rows(source, gain):
    wide = source.astype(jnp.float32)
    return wide * lax.rsqrt(lax.optimization_barrier(jnp.mean(wide * wide, axis=-1, keepdims=True)) + epsilon) * gain

def reference(tokens, lengths, key_cache, value_cache, attn_gain, w_query, w_key, w_value, mix_lambda, head_gain, w_out, ffn_gain, w_gate, w_up, w_down, routes, route_weights):
    groups = SEQS // SEQ_DEV
    columns = HEADS * VDIM
    normed = norm_rows(tokens, attn_gain).astype(jnp.bfloat16)
    queries = jnp.dot(normed, w_query.reshape(D, columns), preferred_element_type=jnp.float32).astype(jnp.bfloat16)
    key_new = jnp.dot(normed, w_key.reshape(D, columns), preferred_element_type=jnp.float32).astype(jnp.bfloat16)
    value_new = jnp.dot(normed, w_value.reshape(D, columns), preferred_element_type=jnp.float32).astype(jnp.bfloat16)
    halves = (lax.iota(jnp.int32, VDIM) < HALF).astype(jnp.float32)
    selector = jnp.stack([halves, 1.0 - halves])
    score_scale = HALF ** (-0.5)
    positions = lax.iota(jnp.int32, LEN)

    def attend(blocks):
        query_rows, fresh_keys, fresh_values, key_rows, value_rows, seq_lengths = blocks
        query_wide = query_rows.astype(jnp.float32)[:, :, None, :] * selector[None, None]
        scores = jnp.einsum('shcd,slhd->shcl', query_wide, key_rows.astype(jnp.float32)) * score_scale
        own_scores = jnp.einsum('shcd,shd->shc', query_wide, fresh_keys.astype(jnp.float32)) * score_scale
        live_mask = (positions[None, :] < seq_lengths[:, None])[:, None, None, :]
        scores = jnp.where(live_mask, scores, -jnp.inf)
        peak = jnp.maximum(lax.optimization_barrier(jnp.max(scores, axis=-1)), own_scores)
        weights = jnp.exp(scores - peak[..., None])
        own_weight = jnp.exp(own_scores - peak)
        denominator = lax.optimization_barrier(jnp.sum(weights, axis=-1)) + own_weight
        shares = weights / denominator[..., None]
        own_share = own_weight / denominator
        balance = mix_lambda[None, :]
        mix_weights = (shares[:, :, 0] - balance[..., None] * shares[:, :, 1]).astype(jnp.bfloat16)
        own_mixed = (own_share[:, :, 0] - balance * own_share[:, :, 1]).astype(jnp.bfloat16)
        output = jnp.einsum('shl,slhd->shd', mix_weights.astype(jnp.float32), value_rows.astype(jnp.float32))
        return output + own_mixed.astype(jnp.float32)[..., None] * fresh_values.astype(jnp.float32)
    grouped = lax.map(attend, (queries.reshape(groups, SEQ_DEV, HEADS, VDIM), key_new.reshape(groups, SEQ_DEV, HEADS, VDIM), value_new.reshape(groups, SEQ_DEV, HEADS, VDIM), key_cache.reshape(groups, SEQ_DEV, LEN, HEADS, VDIM), value_cache.reshape(groups, SEQ_DEV, LEN, HEADS, VDIM), lengths.reshape(groups, SEQ_DEV)))
    heads_out = grouped.reshape(SEQS, HEADS, VDIM)
    normed_heads = (heads_out * lax.rsqrt(lax.optimization_barrier(jnp.mean(heads_out * heads_out, axis=-1, keepdims=True)) + epsilon) * head_gain * branch_scale).astype(jnp.bfloat16)
    parts = jnp.einsum('sgk,gkd->sgd', normed_heads.reshape(SEQS, N_TP, GROUP_HEADS * VDIM).astype(jnp.float32), w_out.reshape(N_TP, GROUP_HEADS * VDIM, D).astype(jnp.float32))
    attention = lax.optimization_barrier(jnp.sum(lax.optimization_barrier(parts.astype(jnp.bfloat16)).astype(jnp.float32), axis=1))
    residual = (tokens.astype(jnp.float32) + attention).astype(jnp.bfloat16)
    normed_ffn = norm_rows(residual, ffn_gain).astype(jnp.bfloat16)
    entries = routes.reshape(groups, SEQ_DEV * TOP)
    onehot = (entries[..., None] == lax.iota(jnp.int32, EXPERTS)[None, None, :]).astype(jnp.int32)
    entry_slot = lax.optimization_barrier(jnp.sum((jnp.cumsum(onehot, axis=1) - onehot) * onehot, axis=-1))
    target = (entries * CAP + entry_slot).astype(jnp.int32)
    placing = (lax.iota(jnp.int32, EXPERTS * CAP)[None, :, None] == target[:, None, :]).astype(jnp.float32)
    repeated = jnp.repeat(normed_ffn.reshape(groups, SEQ_DEV, D), TOP, axis=1).astype(jnp.float32)
    outgoing = jnp.einsum('gtr,grd->gtd', placing, repeated).astype(jnp.bfloat16)
    by_expert = outgoing.reshape(groups, EXPERTS, CAP, D).transpose(1, 0, 2, 3).reshape(EXPERTS, groups * CAP, D)

    def expert(blocks):
        arrived, gate_weight, up_weight, down_weight = blocks
        gate_value = jnp.minimum(jnp.dot(arrived, gate_weight, preferred_element_type=jnp.float32), clamp_limit)
        up_value = jnp.clip(jnp.dot(arrived, up_weight, preferred_element_type=jnp.float32), -clamp_limit, clamp_limit)
        activated = ((up_value + 1.0) * gate_value * jax.nn.sigmoid(sigmoid_slope * gate_value)).astype(jnp.bfloat16)
        pieces = jnp.einsum('rgf,gfd->rgd', activated.reshape(-1, N_TP, FF_DEV).astype(jnp.float32), down_weight.reshape(N_TP, FF_DEV, D).astype(jnp.float32))
        summed = lax.optimization_barrier(jnp.sum(lax.optimization_barrier(pieces.astype(jnp.bfloat16)).astype(jnp.float32), axis=1))
        return summed.astype(jnp.bfloat16)
    results = lax.map(expert, (by_expert, w_gate, w_up, w_down))
    returned = results.reshape(EXPERTS, groups, CAP, D).transpose(1, 0, 2, 3).reshape(groups, EXPERTS * CAP, D)
    chosen = (lax.iota(jnp.int32, EXPERTS * CAP)[None, None, None, :] == target.reshape(groups, SEQ_DEV, TOP)[..., None]).astype(jnp.float32)
    combine = lax.optimization_barrier(jnp.sum(route_weights.reshape(groups, SEQ_DEV, TOP, 1) * chosen, axis=2))
    expert_sum = jnp.einsum('gsr,grd->gsd', combine, returned.astype(jnp.float32), precision=lax.Precision.HIGHEST)
    return (residual.astype(jnp.float32) + expert_sum.reshape(SEQS, D)).astype(jnp.bfloat16)
```

```python
import jax
import jax.numpy as jnp
from jax import lax
from jax.sharding import PartitionSpec as P

epsilon = 1e-06
clamp_limit = 7.0
sigmoid_slope = 1.702
branch_scale = 0.2


def norm_rows(source, gain):
    wide = source.astype(jnp.float32)
    return wide * lax.rsqrt(jnp.mean(wide * wide, axis=-1, keepdims=True) + epsilon) * gain


def mixed_weights(scores, own_scores, mix_lambda):
    peak = jnp.maximum(jnp.max(scores, axis=-1), own_scores)
    weights = jnp.exp(scores - peak[..., None])
    own_weight = jnp.exp(own_scores - peak)
    denominator = jnp.sum(weights, axis=-1) + own_weight
    shares = weights / denominator[..., None]
    own_share = own_weight / denominator
    balance = mix_lambda[None, :]
    mix_weights = (shares[:, :, 0] - balance[..., None] * shares[:, :, 1]).astype(jnp.bfloat16)
    own_mixed = (own_share[:, :, 0] - balance * own_share[:, :, 1]).astype(jnp.bfloat16)
    return (mix_weights, own_mixed)


def per_device(
    tokens,
    lengths,
    key_cache,
    value_cache,
    attn_gain,
    w_query,
    w_key,
    w_value,
    mix_lambda,
    head_gain,
    w_out,
    ffn_gain,
    w_gate,
    w_up,
    w_down,
    routes,
    route_weights,
):
    seq_dev, model_width = tokens.shape
    group_heads = w_query.shape[1]
    head_width = w_query.shape[2]
    half_width = head_width // 2
    columns = group_heads * head_width
    cache_len = key_cache.shape[1]
    normed = norm_rows(tokens, attn_gain).astype(jnp.bfloat16)
    queries = (
        jnp.dot(normed, w_query.reshape(model_width, columns), preferred_element_type=jnp.float32)
        .astype(jnp.bfloat16)
        .reshape(seq_dev, group_heads, head_width)
    )
    key_new = (
        jnp.dot(normed, w_key.reshape(model_width, columns), preferred_element_type=jnp.float32)
        .astype(jnp.bfloat16)
        .reshape(seq_dev, group_heads, head_width)
    )
    value_new = (
        jnp.dot(normed, w_value.reshape(model_width, columns), preferred_element_type=jnp.float32)
        .astype(jnp.bfloat16)
        .reshape(seq_dev, group_heads, head_width)
    )
    halves = (lax.iota(jnp.int32, head_width) < half_width).astype(jnp.bfloat16)
    stacked_query = jnp.stack([queries * halves, queries * (1 - halves)], axis=2)
    score_scale = half_width ** (-0.5)
    own_scores = (
        jnp.einsum("shcd,shd->shc", stacked_query, key_new, preferred_element_type=jnp.float32)
        * score_scale
    )
    positions = lax.iota(jnp.int32, cache_len)
    live_mask = (positions[None, :] < lengths[:, None])[:, None, None, :]
    scores = (
        jnp.einsum("shcd,slhd->shcl", stacked_query, key_cache, preferred_element_type=jnp.float32)
        * score_scale
    )
    scores = jnp.where(live_mask, scores, -jnp.inf)
    mix_weights, own_mixed = mixed_weights(scores, own_scores, mix_lambda)
    heads_out = jnp.einsum(
        "shl,slhd->shd", mix_weights, value_cache, preferred_element_type=jnp.float32
    )
    heads_out = heads_out + own_mixed.astype(jnp.float32)[..., None] * value_new.astype(jnp.float32)
    normed_heads = (
        heads_out
        * lax.rsqrt(jnp.mean(heads_out * heads_out, axis=-1, keepdims=True) + epsilon)
        * head_gain
        * branch_scale
    ).astype(jnp.bfloat16)
    partial_value = jnp.dot(
        normed_heads.reshape(seq_dev, columns),
        w_out.reshape(columns, model_width),
        preferred_element_type=jnp.float32,
    )
    partial_value = partial_value.astype(jnp.bfloat16)
    own_core = lax.axis_index("core")
    rows_y = lax.axis_size("y")
    width = model_width // (2 * rows_y)
    experts = lax.axis_size("ep")
    top_count = routes.shape[1]
    capacity = min(seq_dev, 2 * seq_dev * top_count // experts)

    def halves_of(source):
        blocks = source.reshape(source.shape[0], rows_y, 2, width)
        kept = lax.dynamic_index_in_dim(blocks, own_core, 2, keepdims=False)
        sent = lax.dynamic_index_in_dim(blocks, 1 - own_core, 2, keepdims=False)
        return kept, sent

    def swap_cores(source):
        return lax.ppermute(source, "core", [(0, 1), (1, 0)])

    def pair_sum(source):
        kept, sent = halves_of(source)
        arrived = swap_cores(sent)
        return (kept.astype(jnp.float32) + arrived.astype(jnp.float32)).astype(jnp.bfloat16)

    pair = pair_sum(partial_value)
    if rows_y == 2:
        other = lax.ppermute(pair, "y", [(0, 1), (1, 0)])
        attention = pair.astype(jnp.float32) + other.astype(jnp.float32)
    else:
        attention = jnp.sum(lax.all_gather(pair, "y").astype(jnp.float32), axis=0)
    own_tokens, _ = halves_of(tokens)
    residual = (own_tokens.astype(jnp.float32) + attention).astype(jnp.bfloat16)
    half_width_all = rows_y * width
    flat_residual = residual.reshape(seq_dev, half_width_all)
    if capacity < seq_dev:
        entries = routes.reshape(-1)
        onehot = (entries[:, None] == lax.iota(jnp.int32, experts)[None, :]).astype(jnp.int32)
        entry_slot = jnp.sum((jnp.cumsum(onehot, axis=0) - onehot) * onehot, axis=-1)
        target = (entries * capacity + entry_slot).reshape(seq_dev, top_count)
        slot_ids = lax.iota(jnp.int32, experts * capacity)
        chosen = (target[..., None] == slot_ids[None, None, :]).astype(jnp.float32)
        placing = jnp.sum(chosen, axis=1).astype(jnp.bfloat16)
        outgoing = lax.dot_general(
            placing, flat_residual, (((0,), (0,)), ((), ())), preferred_element_type=jnp.float32
        ).astype(jnp.bfloat16)
        outgoing = outgoing.reshape(experts, capacity, half_width_all)
    else:
        outgoing = jnp.broadcast_to(flat_residual[None], (experts, seq_dev, half_width_all))
    arrived = lax.all_to_all(outgoing, "ep", split_axis=0, concat_axis=0, tiled=True)
    own_half = arrived.reshape(experts * capacity, rows_y, width)
    other_half = swap_cores(own_half)
    flat_rows = jnp.where(
        own_core == 0,
        jnp.stack([own_half, other_half], axis=2),
        jnp.stack([other_half, own_half], axis=2),
    ).reshape(experts * capacity, model_width)
    normed_ffn = norm_rows(flat_rows, ffn_gain).astype(jnp.bfloat16)
    gate_value = jnp.minimum(
        jnp.dot(normed_ffn, w_gate[0], preferred_element_type=jnp.float32), clamp_limit
    )
    up_value = jnp.clip(
        jnp.dot(normed_ffn, w_up[0], preferred_element_type=jnp.float32), -clamp_limit, clamp_limit
    )
    activated = ((up_value + 1.0) * gate_value * jax.nn.sigmoid(sigmoid_slope * gate_value)).astype(
        jnp.bfloat16
    )
    pieces = jnp.dot(activated, w_down[0], preferred_element_type=jnp.float32).astype(jnp.bfloat16)
    pieces = pair_sum(pieces).reshape(experts, capacity, rows_y, width)
    pieces = pieces.transpose(0, 2, 1, 3).reshape(experts * rows_y, capacity, width)
    returned = lax.all_to_all(pieces, ("ep", "y"), split_axis=0, concat_axis=0, tiled=True)
    returned = returned.reshape(experts, rows_y, capacity, width).astype(jnp.float32)
    expert_out = jnp.sum(returned, axis=1).astype(jnp.bfloat16).astype(jnp.float32)
    if capacity < seq_dev:
        combine = jnp.sum(route_weights[..., None] * chosen, axis=1)
        expert_sum = jnp.dot(
            combine, expert_out.reshape(experts * capacity, width), precision=lax.Precision.HIGHEST
        )
    else:
        named = routes[..., None] == lax.iota(jnp.int32, experts)[None, None, :]
        weights = jnp.sum(jnp.where(named, route_weights[..., None], 0.0), axis=1)
        expert_sum = jnp.sum(weights.T[:, :, None] * expert_out, axis=0)
    own_columns = lax.dynamic_index_in_dim(residual, lax.axis_index("y"), 1, keepdims=False)
    return (own_columns.astype(jnp.float32) + expert_sum).astype(jnp.bfloat16)


def solution(mesh):
    experts, shards = mesh.shape["ep"], mesh.shape["tp"]
    split = jax.sharding.Mesh(mesh.devices.reshape(experts, shards // 2, 2), ("ep", "y", "core"))
    tp = ("y", "core")
    placed = (
        P("ep", None),
        P("ep"),
        P("ep", None, tp, None),
        P("ep", None, tp, None),
        P(),
        P(None, tp, None),
        P(None, tp, None),
        P(None, tp, None),
        P(tp),
        P(),
        P(tp, None, None),
        P(),
        P("ep", None, tp),
        P("ep", None, tp),
        P("ep", tp, None),
        P("ep", None),
        P("ep", None),
    )
    return jax.shard_map(
        per_device, mesh=split, in_specs=placed, out_specs=P("ep", tp), check_vma=False
    )
```

```python
import jax
import jax.numpy as jnp
from jax import lax
from jax.experimental import pallas as pl
from jax.experimental.pallas import tpu as pltpu
from jax.sharding import PartitionSpec as P

epsilon = 1e-06
clamp_limit = 7.0
sigmoid_slope = 1.702
branch_scale = 0.2
group_rows = 8


def norm_rows(source, gain):
    wide = source.astype(jnp.float32)
    return wide * lax.rsqrt(jnp.mean(wide * wide, axis=-1, keepdims=True) + epsilon) * gain


def attention_kernel(
    lengths_hbm,
    lambda_hbm,
    tokens_hbm,
    gain_hbm,
    head_gain_hbm,
    query_hbm,
    key_hbm,
    value_hbm,
    keys_hbm,
    values_hbm,
    out_hbm,
    kept_ref,
    sent_ref,
    lengths_ref,
    lambda_ref,
    tokens_ref,
    gain_ref,
    head_gain_ref,
    weights_ref,
    keys_ref,
    values_ref,
    out_ref,
    wide_ref,
    query_ref,
    scores_ref,
    peak_ref,
    total_ref,
    heads_ref,
    small_sem,
    large_sem,
):
    seqs, positions, head_width = keys_ref.shape
    model_width = tokens_ref.shape[1]
    heads = query_hbm.shape[0] // model_width
    rows_y, width = kept_ref.shape[0], kept_ref.shape[2]
    lanes = 128
    rows = seqs * group_rows
    f32, bf16 = jnp.float32, jnp.bfloat16

    small = [
        pltpu.make_async_copy(source, target, small_sem.at[i])
        for i, (source, target) in enumerate(
            (
                (tokens_hbm, tokens_ref),
                (gain_hbm, gain_ref),
                (lengths_hbm, lengths_ref),
                (lambda_hbm, lambda_ref),
                (head_gain_hbm, head_gain_ref),
            )
        )
    ]
    for copy in small:
        copy.start()
    large = [
        pltpu.make_async_copy(source, target, large_sem.at[i])
        for i, (source, target) in enumerate(
            (
                (query_hbm, weights_ref.at[0]),
                (key_hbm, weights_ref.at[1]),
                (value_hbm, weights_ref.at[2]),
                (keys_hbm, keys_ref),
                (values_hbm, values_ref),
                (out_hbm, out_ref),
            )
        )
    ]
    for copy in large:
        copy.start()
    for copy in small:
        copy.wait()
    normed = norm_rows(tokens_ref[...], gain_ref[...]).astype(bf16)
    spread = (
        lax.broadcasted_iota(jnp.int32, (lanes, heads * lanes), 1) // heads
        == lax.broadcasted_iota(jnp.int32, (lanes, heads * lanes), 0)
    ).astype(bf16)
    lane_head = lax.broadcasted_iota(jnp.int32, (seqs, heads * lanes), 1) % heads
    for block in range(model_width // lanes):
        part = jnp.dot(
            normed[:, block * lanes : (block + 1) * lanes], spread, preferred_element_type=f32
        )
        columns = slice(block * heads * lanes, (block + 1) * heads * lanes)
        for h in range(heads):
            wide_ref[h * seqs : (h + 1) * seqs, columns] = jnp.where(
                lane_head == h, part, 0.0
            ).astype(bf16)

    row_ids = lax.broadcasted_iota(jnp.int32, (rows, heads * seqs), 0)
    column_ids = lax.broadcasted_iota(jnp.int32, (rows, heads * seqs), 1)
    placing = (
        (column_ids % seqs == row_ids // group_rows)
        & (column_ids // seqs == (row_ids % group_rows) // 2 % heads)
    ).astype(bf16)

    def project(i):
        large[i].wait()
        product = jnp.dot(wide_ref[...], weights_ref[i], preferred_element_type=f32)
        return jnp.dot(placing, product.astype(bf16), preferred_element_type=f32)

    place = lax.broadcasted_iota(jnp.int32, (rows, head_width), 0) % group_rows
    lane = lax.broadcasted_iota(jnp.int32, (rows, head_width), 1)
    own_half = ((lane < head_width // 2) == (place % 2 == 0)) & (place < 2 * heads)
    queries = jnp.where(own_half, project(0), 0.0) * (head_width // 2) ** (-0.5)
    query_ref[...] = queries
    own_scores = jnp.sum(queries * project(1), axis=-1, keepdims=True)
    value_new = project(2)

    group = lax.broadcasted_iota(jnp.int32, (group_rows, positions), 0)
    spot = lax.broadcasted_iota(jnp.int32, (group_rows, positions), 1)
    own_head = spot % heads == group // 2 % heads
    spot = jnp.where(own_head, spot, positions)

    def folded(source, combine):
        parts = [source[:, i : i + lanes] for i in range(0, positions, lanes)]
        while len(parts) > 1:
            parts = [combine(a, b) for a, b in zip(parts[::2], parts[1::2])]
        return parts[0]

    large[3].wait()
    for s in range(seqs):
        at = slice(s * group_rows, (s + 1) * group_rows)
        scores = lax.dot_general(
            query_ref[at, :].astype(bf16),
            keys_ref[s],
            (((1,), (1,)), ((), ())),
            preferred_element_type=f32,
        )
        scores = jnp.where(spot < lengths_ref[s] * heads, scores, -jnp.inf)
        scores_ref[at, :] = scores
        peak_ref[at, :] = folded(scores, jnp.maximum)

    peak = jnp.maximum(jnp.max(peak_ref[...], axis=-1, keepdims=True), own_scores)
    peak_ref[...] = jnp.broadcast_to(peak, peak_ref.shape)
    for s in range(seqs):
        at = slice(s * group_rows, (s + 1) * group_rows)
        shifted = jnp.exp(scores_ref[at, :] - peak_ref[at, 0:1])
        scores_ref[at, :] = shifted
        total_ref[at, :] = folded(shifted, jnp.add)

    own_weight = jnp.exp(own_scores - peak)
    denominator = jnp.sum(total_ref[...], axis=-1, keepdims=True) + own_weight
    row = lax.broadcasted_iota(jnp.int32, (rows, 1), 0) % group_rows
    factor = jnp.ones((rows, 1), f32)
    for h in range(heads):
        factor = jnp.where(row == 2 * h + 1, -lambda_ref[h], factor)
    factor = factor / denominator
    peak_ref[...] = jnp.broadcast_to(factor, peak_ref.shape)
    total_ref[...] = jnp.broadcast_to(own_weight * factor, peak_ref.shape)
    query_ref[...] = value_new

    def mixed(source):
        return (source + pltpu.roll(source, group_rows - 1, 0)).astype(bf16)

    large[4].wait()
    for s in range(seqs):
        at = slice(s * group_rows, (s + 1) * group_rows)
        weights = mixed(scores_ref[at, :] * peak_ref[at, 0:1])
        own = mixed(total_ref[at, :]).astype(f32)
        heads_ref[at, :] = (
            jnp.dot(weights, values_ref[s], preferred_element_type=f32)
            + own * query_ref[at, :]
        )

    heads_out = heads_ref[...]
    normed_heads = (
        heads_out
        * lax.rsqrt(jnp.mean(heads_out * heads_out, axis=-1, keepdims=True) + epsilon)
        * head_gain_ref[...]
        * branch_scale
    ).astype(bf16)
    picked = []
    taker = lax.broadcasted_iota(jnp.int32, (seqs, rows), 0) * group_rows
    giver = lax.broadcasted_iota(jnp.int32, (seqs, rows), 1)
    for h in range(heads):
        chosen = (giver == taker + 2 * h).astype(bf16)
        picked.append(jnp.dot(chosen, normed_heads, preferred_element_type=f32).astype(bf16))
    joined = jnp.concatenate(picked, axis=1) if heads > 1 else picked[0]
    large[5].wait()
    core = lax.axis_index("core")
    for y in range(rows_y):
        for target, which in ((sent_ref, 1 - core), (kept_ref, core)):
            columns = pl.ds(pl.multiple_of((2 * y + which) * width, width), width)
            target[y] = jnp.dot(
                joined, out_ref[:, columns], preferred_element_type=f32
            ).astype(bf16)


def attend(
    tokens,
    lengths,
    key_cache,
    value_cache,
    attn_gain,
    w_query,
    w_key,
    w_value,
    mix_lambda,
    head_gain,
    w_out,
    rows_y,
):
    seqs, model_width = tokens.shape
    cache_len, heads, head_width = key_cache.shape[1:]
    positions = cache_len * heads
    rows = seqs * group_rows
    width = model_width // (2 * rows_y)
    bf16, f32 = jnp.bfloat16, jnp.float32
    vmem = pl.BlockSpec(memory_space=pltpu.VMEM)
    hbm = pl.BlockSpec(memory_space=pltpu.HBM)
    out = jax.ShapeDtypeStruct((rows_y, seqs, width), bf16)
    return pl.pallas_call(
        attention_kernel,
        out_shape=(out, out),
        in_specs=[hbm] * 11,
        out_specs=(vmem, vmem),
        scratch_shapes=[
            pltpu.SMEM((seqs,), jnp.int32),
            pltpu.SMEM((heads,), f32),
            pltpu.VMEM((seqs, model_width), bf16),
            pltpu.VMEM((1, model_width), f32),
            pltpu.VMEM((1, head_width), f32),
            pltpu.VMEM((3, model_width * heads, head_width), bf16),
            pltpu.VMEM((seqs, positions, head_width), bf16),
            pltpu.VMEM((seqs, positions, head_width), bf16),
            pltpu.VMEM((heads * head_width, model_width), bf16),
            pltpu.VMEM((heads * seqs, heads * model_width), bf16),
            pltpu.VMEM((rows, head_width), f32),
            pltpu.VMEM((rows, positions), f32),
            pltpu.VMEM((rows, 128), f32),
            pltpu.VMEM((rows, 128), f32),
            pltpu.VMEM((rows, head_width), f32),
            pltpu.SemaphoreType.DMA((5,)),
            pltpu.SemaphoreType.DMA((6,)),
        ],
        compiler_params=pltpu.CompilerParams(vmem_limit_bytes=attention_vmem),
        cost_estimate=pl.CostEstimate(
            flops=attention_flops, bytes_accessed=4 * key_cache.size, transcendentals=0
        ),
        name="attention",
    )(
        lengths,
        mix_lambda,
        tokens,
        attn_gain.reshape(1, model_width),
        head_gain.reshape(1, head_width),
        w_query.reshape(model_width * heads, head_width),
        w_key.reshape(model_width * heads, head_width),
        w_value.reshape(model_width * heads, head_width),
        key_cache.reshape(seqs, positions, head_width),
        value_cache.reshape(seqs, positions, head_width),
        w_out.reshape(heads * head_width, model_width),
    )


attention_vmem = 63 * 1024 * 1024
attention_flops = 4 * 10**9


def per_device(
    tokens,
    lengths,
    key_cache,
    value_cache,
    attn_gain,
    w_query,
    w_key,
    w_value,
    mix_lambda,
    head_gain,
    w_out,
    ffn_gain,
    w_gate,
    w_up,
    w_down,
    routes,
    route_weights,
):
    seq_dev, model_width = tokens.shape
    own_core = lax.axis_index("core")
    rows_y = lax.axis_size("y")
    width = model_width // (2 * rows_y)
    experts = lax.axis_size("ep")
    top_count = routes.shape[1]
    capacity = min(seq_dev, 2 * seq_dev * top_count // experts)

    def halves_of(source):
        blocks = source.reshape(source.shape[0], rows_y, 2, width)
        kept = lax.dynamic_index_in_dim(blocks, own_core, 2, keepdims=False)
        sent = lax.dynamic_index_in_dim(blocks, 1 - own_core, 2, keepdims=False)
        return kept, sent

    def swap_cores(source):
        return lax.ppermute(source, "core", [(0, 1), (1, 0)])

    def add_swapped(kept, sent):
        arrived = swap_cores(sent)
        return (kept.astype(jnp.float32) + arrived.astype(jnp.float32)).astype(jnp.bfloat16)

    kept, sent = attend(
        tokens,
        lengths,
        key_cache,
        value_cache,
        attn_gain,
        w_query,
        w_key,
        w_value,
        mix_lambda,
        head_gain,
        w_out,
        rows_y,
    )
    pair = add_swapped(kept, sent)
    if rows_y == 2:
        other = lax.ppermute(pair, "y", [(0, 1), (1, 0)])
        attention = pair.astype(jnp.float32) + other.astype(jnp.float32)
    else:
        attention = jnp.sum(lax.all_gather(pair, "y").astype(jnp.float32), axis=0)
    attention = attention.transpose(1, 0, 2)
    own_tokens, _ = halves_of(tokens)
    residual = (own_tokens.astype(jnp.float32) + attention).astype(jnp.bfloat16)
    half_width_all = rows_y * width
    flat_residual = residual.reshape(seq_dev, half_width_all)
    if capacity < seq_dev:
        entries = routes.reshape(-1)
        onehot = (entries[:, None] == lax.iota(jnp.int32, experts)[None, :]).astype(jnp.int32)
        entry_slot = jnp.sum((jnp.cumsum(onehot, axis=0) - onehot) * onehot, axis=-1)
        target = (entries * capacity + entry_slot).reshape(seq_dev, top_count)
        slot_ids = lax.iota(jnp.int32, experts * capacity)
        chosen = (target[..., None] == slot_ids[None, None, :]).astype(jnp.float32)
        placing = jnp.sum(chosen, axis=1).astype(jnp.bfloat16)
        outgoing = lax.dot_general(
            placing, flat_residual, (((0,), (0,)), ((), ())), preferred_element_type=jnp.float32
        ).astype(jnp.bfloat16)
        outgoing = outgoing.reshape(experts, capacity, half_width_all)
    else:
        outgoing = jnp.broadcast_to(flat_residual[None], (experts, seq_dev, half_width_all))
    arrived = lax.all_to_all(outgoing, "ep", split_axis=0, concat_axis=0, tiled=True)
    own_half = arrived.reshape(experts * capacity, rows_y, width)
    other_half = swap_cores(own_half)
    flat_rows = jnp.where(
        own_core == 0,
        jnp.stack([own_half, other_half], axis=2),
        jnp.stack([other_half, own_half], axis=2),
    ).reshape(experts * capacity, model_width)
    normed_ffn = norm_rows(flat_rows, ffn_gain).astype(jnp.bfloat16)
    gate_value = jnp.minimum(
        jnp.dot(normed_ffn, w_gate[0], preferred_element_type=jnp.float32), clamp_limit
    )
    up_value = jnp.clip(
        jnp.dot(normed_ffn, w_up[0], preferred_element_type=jnp.float32), -clamp_limit, clamp_limit
    )
    activated = ((up_value + 1.0) * gate_value * jax.nn.sigmoid(sigmoid_slope * gate_value)).astype(
        jnp.bfloat16
    )
    pieces = jnp.dot(activated, w_down[0], preferred_element_type=jnp.float32).astype(jnp.bfloat16)
    pieces = add_swapped(*halves_of(pieces)).reshape(experts, capacity, rows_y, width)
    pieces = pieces.transpose(0, 2, 1, 3).reshape(experts * rows_y, capacity, width)
    returned = lax.all_to_all(pieces, ("ep", "y"), split_axis=0, concat_axis=0, tiled=True)
    returned = returned.reshape(experts, rows_y, capacity, width).astype(jnp.float32)
    expert_out = jnp.sum(returned, axis=1).astype(jnp.bfloat16).astype(jnp.float32)
    if capacity < seq_dev:
        combine = jnp.sum(route_weights[..., None] * chosen, axis=1)
        expert_sum = jnp.dot(
            combine, expert_out.reshape(experts * capacity, width), precision=lax.Precision.HIGHEST
        )
    else:
        named = routes[..., None] == lax.iota(jnp.int32, experts)[None, None, :]
        weights = jnp.sum(jnp.where(named, route_weights[..., None], 0.0), axis=1)
        expert_sum = jnp.sum(weights.T[:, :, None] * expert_out, axis=0)
    own_columns = lax.dynamic_index_in_dim(residual, lax.axis_index("y"), 1, keepdims=False)
    return (own_columns.astype(jnp.float32) + expert_sum).astype(jnp.bfloat16)


def solution(mesh):
    experts, shards = mesh.shape["ep"], mesh.shape["tp"]
    split = jax.sharding.Mesh(mesh.devices.reshape(experts, shards // 2, 2), ("ep", "y", "core"))
    tp = ("y", "core")
    placed = (
        P("ep", None),
        P("ep"),
        P("ep", None, tp, None),
        P("ep", None, tp, None),
        P(),
        P(None, tp, None),
        P(None, tp, None),
        P(None, tp, None),
        P(tp),
        P(),
        P(tp, None, None),
        P(),
        P("ep", None, tp),
        P("ep", None, tp),
        P("ep", tp, None),
        P("ep", None),
        P("ep", None),
    )
    return jax.shard_map(
        per_device, mesh=split, in_specs=placed, out_specs=P("ep", tp), check_vma=False
    )
```

```python
import jax
import jax.numpy as jnp
from jax import lax
from jax.experimental import pallas as pl
from jax.experimental.pallas import tpu as pltpu
from jax.sharding import PartitionSpec as P

epsilon = 1e-06
clamp_limit = 7.0
sigmoid_slope = 1.702
branch_scale = 0.2
group_rows = 8


def norm_rows(source, gain):
    wide = source.astype(jnp.float32)
    return wide * lax.rsqrt(jnp.mean(wide * wide, axis=-1, keepdims=True) + epsilon) * gain


def attention_kernel(
    lengths_hbm,
    lambda_hbm,
    tokens_hbm,
    gain_hbm,
    head_gain_hbm,
    query_hbm,
    key_hbm,
    value_hbm,
    keys_hbm,
    values_hbm,
    out_hbm,
    kept_ref,
    sent_ref,
    lengths_ref,
    lambda_ref,
    tokens_ref,
    gain_ref,
    head_gain_ref,
    weights_ref,
    keys_ref,
    values_ref,
    out_ref,
    wide_ref,
    query_ref,
    scores_ref,
    peak_ref,
    total_ref,
    heads_ref,
    small_sem,
    large_sem,
):
    seqs, positions, head_width = keys_ref.shape
    model_width = tokens_ref.shape[1]
    heads = query_hbm.shape[0] // model_width
    rows_y, width = kept_ref.shape[0], kept_ref.shape[2]
    lanes = 128
    rows = seqs * group_rows
    f32, bf16 = jnp.float32, jnp.bfloat16

    small = [
        pltpu.make_async_copy(source, target, small_sem.at[i])
        for i, (source, target) in enumerate(
            (
                (tokens_hbm, tokens_ref),
                (gain_hbm, gain_ref),
                (lengths_hbm, lengths_ref),
                (lambda_hbm, lambda_ref),
                (head_gain_hbm, head_gain_ref),
            )
        )
    ]
    for copy in small:
        copy.start()
    large = [
        pltpu.make_async_copy(source, target, large_sem.at[i])
        for i, (source, target) in enumerate(
            (
                (query_hbm, weights_ref.at[0]),
                (key_hbm, weights_ref.at[1]),
                (value_hbm, weights_ref.at[2]),
                (keys_hbm, keys_ref),
                (values_hbm, values_ref),
                (out_hbm, out_ref),
            )
        )
    ]
    for i in (0, 1, 2, 3):
        large[i].start()
    for copy in small:
        copy.wait()
    large[4].start()
    large[5].start()
    normed = norm_rows(tokens_ref[...], gain_ref[...]).astype(bf16)
    spread = (
        lax.broadcasted_iota(jnp.int32, (lanes, heads * lanes), 1) // heads
        == lax.broadcasted_iota(jnp.int32, (lanes, heads * lanes), 0)
    ).astype(bf16)
    lane_head = lax.broadcasted_iota(jnp.int32, (seqs, heads * lanes), 1) % heads
    for block in range(model_width // lanes):
        part = jnp.dot(
            normed[:, block * lanes : (block + 1) * lanes], spread, preferred_element_type=f32
        )
        columns = slice(block * heads * lanes, (block + 1) * heads * lanes)
        for h in range(heads):
            wide_ref[h * seqs : (h + 1) * seqs, columns] = jnp.where(
                lane_head == h, part, 0.0
            ).astype(bf16)

    row_ids = lax.broadcasted_iota(jnp.int32, (rows, heads * seqs), 0)
    column_ids = lax.broadcasted_iota(jnp.int32, (rows, heads * seqs), 1)
    placing = (
        (column_ids % seqs == row_ids // group_rows)
        & (column_ids // seqs == (row_ids % group_rows) // 2 % heads)
    ).astype(bf16)

    def project(i):
        large[i].wait()
        product = jnp.dot(wide_ref[...], weights_ref[i], preferred_element_type=f32)
        return jnp.dot(placing, product.astype(bf16), preferred_element_type=f32)

    place = lax.broadcasted_iota(jnp.int32, (rows, head_width), 0) % group_rows
    lane = lax.broadcasted_iota(jnp.int32, (rows, head_width), 1)
    own_half = ((lane < head_width // 2) == (place % 2 == 0)) & (place < 2 * heads)
    queries = jnp.where(own_half, project(0), 0.0) * (head_width // 2) ** (-0.5)
    query_ref[...] = queries
    own_scores = jnp.sum(queries * project(1), axis=-1, keepdims=True)
    value_new = project(2)

    group = lax.broadcasted_iota(jnp.int32, (group_rows, positions), 0)
    spot = lax.broadcasted_iota(jnp.int32, (group_rows, positions), 1)
    own_head = spot % heads == group // 2 % heads
    spot = jnp.where(own_head, spot, positions)

    def folded(source, combine):
        parts = [source[:, i : i + lanes] for i in range(0, positions, lanes)]
        while len(parts) > 1:
            parts = [combine(a, b) for a, b in zip(parts[::2], parts[1::2])]
        return parts[0]

    large[3].wait()
    for s in range(seqs):
        at = slice(s * group_rows, (s + 1) * group_rows)
        scores = lax.dot_general(
            query_ref[at, :].astype(bf16),
            keys_ref[s],
            (((1,), (1,)), ((), ())),
            preferred_element_type=f32,
        )
        scores = jnp.where(spot < lengths_ref[s] * heads, scores, -jnp.inf)
        scores_ref[at, :] = scores
        peak_ref[at, :] = folded(scores, jnp.maximum)

    peak = jnp.maximum(jnp.max(peak_ref[...], axis=-1, keepdims=True), own_scores)
    peak_ref[...] = jnp.broadcast_to(peak, peak_ref.shape)
    for s in range(seqs):
        at = slice(s * group_rows, (s + 1) * group_rows)
        shifted = jnp.exp(scores_ref[at, :] - peak_ref[at, 0:1])
        scores_ref[at, :] = shifted
        total_ref[at, :] = folded(shifted, jnp.add)

    own_weight = jnp.exp(own_scores - peak)
    denominator = jnp.sum(total_ref[...], axis=-1, keepdims=True) + own_weight
    row = lax.broadcasted_iota(jnp.int32, (rows, 1), 0) % group_rows
    factor = jnp.ones((rows, 1), f32)
    for h in range(heads):
        factor = jnp.where(row == 2 * h + 1, -lambda_ref[h], factor)
    factor = factor / denominator
    peak_ref[...] = jnp.broadcast_to(factor, peak_ref.shape)
    total_ref[...] = jnp.broadcast_to(own_weight * factor, peak_ref.shape)
    query_ref[...] = value_new

    def mixed(source):
        return (source + pltpu.roll(source, group_rows - 1, 0)).astype(bf16)

    large[4].wait()
    for s in range(seqs):
        at = slice(s * group_rows, (s + 1) * group_rows)
        weights = mixed(scores_ref[at, :] * peak_ref[at, 0:1])
        own = mixed(total_ref[at, :]).astype(f32)
        heads_ref[at, :] = (
            jnp.dot(weights, values_ref[s], preferred_element_type=f32)
            + own * query_ref[at, :]
        )

    heads_out = heads_ref[...]
    normed_heads = (
        heads_out
        * lax.rsqrt(jnp.mean(heads_out * heads_out, axis=-1, keepdims=True) + epsilon)
        * head_gain_ref[...]
        * branch_scale
    ).astype(bf16)
    picked = []
    taker = lax.broadcasted_iota(jnp.int32, (seqs, rows), 0) * group_rows
    giver = lax.broadcasted_iota(jnp.int32, (seqs, rows), 1)
    for h in range(heads):
        chosen = (giver == taker + 2 * h).astype(bf16)
        picked.append(jnp.dot(chosen, normed_heads, preferred_element_type=f32).astype(bf16))
    joined = jnp.concatenate(picked, axis=1) if heads > 1 else picked[0]
    large[5].wait()
    core = lax.axis_index("core")
    for y in range(rows_y):
        for target, which in ((sent_ref, 1 - core), (kept_ref, core)):
            columns = pl.ds(pl.multiple_of((2 * y + which) * width, width), width)
            target[y] = jnp.dot(
                joined, out_ref[:, columns], preferred_element_type=f32
            ).astype(bf16)


def attend(
    tokens,
    lengths,
    key_cache,
    value_cache,
    attn_gain,
    w_query,
    w_key,
    w_value,
    mix_lambda,
    head_gain,
    w_out,
    rows_y,
):
    seqs, model_width = tokens.shape
    cache_len, heads, head_width = key_cache.shape[1:]
    positions = cache_len * heads
    rows = seqs * group_rows
    width = model_width // (2 * rows_y)
    bf16, f32 = jnp.bfloat16, jnp.float32
    vmem = pl.BlockSpec(memory_space=pltpu.VMEM)
    hbm = pl.BlockSpec(memory_space=pltpu.HBM)
    out = jax.ShapeDtypeStruct((rows_y, seqs, width), bf16)
    return pl.pallas_call(
        attention_kernel,
        out_shape=(out, out),
        in_specs=[hbm] * 11,
        out_specs=(vmem, vmem),
        scratch_shapes=[
            pltpu.SMEM((seqs,), jnp.int32),
            pltpu.SMEM((heads,), f32),
            pltpu.VMEM((seqs, model_width), bf16),
            pltpu.VMEM((1, model_width), f32),
            pltpu.VMEM((1, head_width), f32),
            pltpu.VMEM((3, model_width * heads, head_width), bf16),
            pltpu.VMEM((seqs, positions, head_width), bf16),
            pltpu.VMEM((seqs, positions, head_width), bf16),
            pltpu.VMEM((heads * head_width, model_width), bf16),
            pltpu.VMEM((heads * seqs, heads * model_width), bf16),
            pltpu.VMEM((rows, head_width), f32),
            pltpu.VMEM((rows, positions), f32),
            pltpu.VMEM((rows, 128), f32),
            pltpu.VMEM((rows, 128), f32),
            pltpu.VMEM((rows, head_width), f32),
            pltpu.SemaphoreType.DMA((5,)),
            pltpu.SemaphoreType.DMA((6,)),
        ],
        compiler_params=pltpu.CompilerParams(vmem_limit_bytes=attention_vmem),
        cost_estimate=pl.CostEstimate(
            flops=attention_flops, bytes_accessed=4 * key_cache.size, transcendentals=0
        ),
        name="attention",
    )(
        lengths,
        mix_lambda,
        tokens,
        attn_gain.reshape(1, model_width),
        head_gain.reshape(1, head_width),
        w_query.reshape(model_width * heads, head_width),
        w_key.reshape(model_width * heads, head_width),
        w_value.reshape(model_width * heads, head_width),
        key_cache.reshape(seqs, positions, head_width),
        value_cache.reshape(seqs, positions, head_width),
        w_out.reshape(heads * head_width, model_width),
    )


attention_vmem = 63 * 1024 * 1024
attention_flops = 4 * 10**9


def expert_kernel(own_ref, other_ref, gain_ref, gate_ref, up_ref, down_ref, kept_ref, sent_ref):
    rows_y, _, width = kept_ref.shape
    model_width = gain_ref.shape[1]
    f32, bf16 = jnp.float32, jnp.bfloat16
    core = lax.axis_index("core")
    sides = ((own_ref, core), (other_ref, 1 - core))

    def columns(y, which):
        return pl.ds(pl.multiple_of((2 * y + which) * width, width), width)

    total = 0.0
    for source, _ in sides:
        wide = source[...].astype(f32)
        total = total + jnp.sum(wide * wide, axis=-1, keepdims=True)
    scale = lax.rsqrt(total / model_width + epsilon)
    gate_value, up_value = 0.0, 0.0
    for source, which in sides:
        for y in range(rows_y):
            at = columns(y, which)
            wide = source[:, y * width : (y + 1) * width].astype(f32)
            normed = (wide * scale * gain_ref[:, at]).astype(bf16)
            gate_value = gate_value + jnp.dot(normed, gate_ref[at, :], preferred_element_type=f32)
            up_value = up_value + jnp.dot(normed, up_ref[at, :], preferred_element_type=f32)
    gate_value = jnp.minimum(gate_value, clamp_limit)
    up_value = jnp.clip(up_value, -clamp_limit, clamp_limit)
    activated = ((up_value + 1.0) * gate_value * jax.nn.sigmoid(sigmoid_slope * gate_value)).astype(
        bf16
    )
    for target, which in ((sent_ref, 1 - core), (kept_ref, core)):
        for y in range(rows_y):
            target[y] = jnp.dot(
                activated, down_ref[:, columns(y, which)], preferred_element_type=f32
            ).astype(bf16)


def apply_expert(own, other, ffn_gain, w_gate, w_up, w_down, rows_y):
    rows, half = own.shape
    model_width, hidden = w_gate.shape
    out = jax.ShapeDtypeStruct((rows_y, rows, half // rows_y), jnp.bfloat16)
    vmem = pl.BlockSpec(memory_space=pltpu.VMEM)
    return pl.pallas_call(
        expert_kernel,
        out_shape=(out, out),
        in_specs=[vmem] * 6,
        out_specs=(vmem, vmem),
        compiler_params=pltpu.CompilerParams(vmem_limit_bytes=expert_vmem),
        cost_estimate=pl.CostEstimate(
            flops=6 * rows * model_width * hidden,
            bytes_accessed=6 * model_width * hidden,
            transcendentals=rows * hidden,
        ),
        name="expert",
    )(own, other, ffn_gain.reshape(1, model_width), w_gate, w_up, w_down)


expert_vmem = 24 * 1024 * 1024


def per_device(
    tokens,
    lengths,
    key_cache,
    value_cache,
    attn_gain,
    w_query,
    w_key,
    w_value,
    mix_lambda,
    head_gain,
    w_out,
    ffn_gain,
    w_gate,
    w_up,
    w_down,
    routes,
    route_weights,
):
    seq_dev, model_width = tokens.shape
    own_core = lax.axis_index("core")
    rows_y = lax.axis_size("y")
    width = model_width // (2 * rows_y)
    experts = lax.axis_size("ep")
    top_count = routes.shape[1]
    capacity = min(seq_dev, 2 * seq_dev * top_count // experts)

    def halves_of(source):
        blocks = source.reshape(source.shape[0], rows_y, 2, width)
        kept = lax.dynamic_index_in_dim(blocks, own_core, 2, keepdims=False)
        sent = lax.dynamic_index_in_dim(blocks, 1 - own_core, 2, keepdims=False)
        return kept, sent

    def swap_cores(source):
        return lax.ppermute(source, "core", [(0, 1), (1, 0)])

    def add_swapped(kept, sent):
        arrived = swap_cores(sent)
        return (kept.astype(jnp.float32) + arrived.astype(jnp.float32)).astype(jnp.bfloat16)

    kept, sent = attend(
        tokens,
        lengths,
        key_cache,
        value_cache,
        attn_gain,
        w_query,
        w_key,
        w_value,
        mix_lambda,
        head_gain,
        w_out,
        rows_y,
    )
    pair = add_swapped(kept, sent)
    if rows_y == 2:
        other = lax.ppermute(pair, "y", [(0, 1), (1, 0)])
        attention = pair.astype(jnp.float32) + other.astype(jnp.float32)
    else:
        attention = jnp.sum(lax.all_gather(pair, "y").astype(jnp.float32), axis=0)
    attention = attention.transpose(1, 0, 2)
    own_tokens, _ = halves_of(tokens)
    residual = (own_tokens.astype(jnp.float32) + attention).astype(jnp.bfloat16)
    half_width_all = rows_y * width
    flat_residual = residual.reshape(seq_dev, half_width_all)
    if capacity < seq_dev:
        entries = routes.reshape(-1)
        onehot = (entries[:, None] == lax.iota(jnp.int32, experts)[None, :]).astype(jnp.int32)
        entry_slot = jnp.sum((jnp.cumsum(onehot, axis=0) - onehot) * onehot, axis=-1)
        target = (entries * capacity + entry_slot).reshape(seq_dev, top_count)
        slot_ids = lax.iota(jnp.int32, experts * capacity)
        chosen = (target[..., None] == slot_ids[None, None, :]).astype(jnp.float32)
        placing = jnp.sum(chosen, axis=1).astype(jnp.bfloat16)
        outgoing = lax.dot_general(
            placing, flat_residual, (((0,), (0,)), ((), ())), preferred_element_type=jnp.float32
        ).astype(jnp.bfloat16)
        outgoing = outgoing.reshape(experts, capacity, half_width_all)
    else:
        outgoing = jnp.broadcast_to(flat_residual[None], (experts, seq_dev, half_width_all))
    arrived = lax.all_to_all(outgoing, "ep", split_axis=0, concat_axis=0, tiled=True)
    own_half = arrived.reshape(experts * capacity, half_width_all)
    kept, sent = apply_expert(
        own_half, swap_cores(own_half), ffn_gain, w_gate[0], w_up[0], w_down[0], rows_y
    )
    pieces = add_swapped(kept, sent).reshape(rows_y * experts, capacity, width)
    returned = lax.all_to_all(pieces, ("y", "ep"), split_axis=0, concat_axis=0, tiled=True)
    returned = returned.reshape(rows_y, experts, capacity, width).astype(jnp.float32)
    expert_out = jnp.sum(returned, axis=0).astype(jnp.bfloat16).astype(jnp.float32)
    if capacity < seq_dev:
        combine = jnp.sum(route_weights[..., None] * chosen, axis=1)
        expert_sum = jnp.dot(
            combine, expert_out.reshape(experts * capacity, width), precision=lax.Precision.HIGHEST
        )
    else:
        named = routes[..., None] == lax.iota(jnp.int32, experts)[None, None, :]
        weights = jnp.sum(jnp.where(named, route_weights[..., None], 0.0), axis=1)
        expert_sum = jnp.sum(weights.T[:, :, None] * expert_out, axis=0)
    own_columns = lax.dynamic_index_in_dim(residual, lax.axis_index("y"), 1, keepdims=False)
    return (own_columns.astype(jnp.float32) + expert_sum).astype(jnp.bfloat16)


def solution(mesh):
    experts, shards = mesh.shape["ep"], mesh.shape["tp"]
    split = jax.sharding.Mesh(mesh.devices.reshape(experts, shards // 2, 2), ("ep", "y", "core"))
    tp = ("y", "core")
    placed = (
        P("ep", None),
        P("ep"),
        P("ep", None, tp, None),
        P("ep", None, tp, None),
        P(),
        P(None, tp, None),
        P(None, tp, None),
        P(None, tp, None),
        P(tp),
        P(),
        P(tp, None, None),
        P(),
        P("ep", None, tp),
        P("ep", None, tp),
        P("ep", tp, None),
        P("ep", None),
        P("ep", None),
    )
    return jax.shard_map(
        per_device, mesh=split, in_specs=placed, out_specs=P("ep", tp), check_vma=False
    )
```

```python
import jax
import jax.numpy as jnp
from jax import lax
from jax.experimental import pallas as pl
from jax.experimental.pallas import tpu as pltpu
from jax.sharding import PartitionSpec as P

epsilon = 1e-06
clamp_limit = 7.0
sigmoid_slope = 1.702
branch_scale = 0.2
group_rows = 8


def norm_rows(source, gain):
    wide = source.astype(jnp.float32)
    return wide * lax.rsqrt(jnp.mean(wide * wide, axis=-1, keepdims=True) + epsilon) * gain


def attention_kernel(
    lengths_hbm,
    lambda_hbm,
    tokens_hbm,
    gain_hbm,
    head_gain_hbm,
    query_hbm,
    key_hbm,
    value_hbm,
    keys_hbm,
    values_hbm,
    out_hbm,
    kept_ref,
    sent_ref,
    lengths_ref,
    lambda_ref,
    tokens_ref,
    gain_ref,
    head_gain_ref,
    weights_ref,
    keys_ref,
    values_ref,
    out_ref,
    wide_ref,
    query_ref,
    scores_ref,
    peak_ref,
    total_ref,
    heads_ref,
    small_sem,
    large_sem,
):
    seqs, positions, head_width = keys_ref.shape
    model_width = tokens_ref.shape[1]
    heads = query_hbm.shape[0] // model_width
    rows_y, width = kept_ref.shape[0], kept_ref.shape[2]
    lanes = 128
    rows = seqs * group_rows
    f32, bf16 = jnp.float32, jnp.bfloat16

    small = [
        pltpu.make_async_copy(source, target, small_sem.at[i])
        for i, (source, target) in enumerate(
            (
                (tokens_hbm, tokens_ref),
                (gain_hbm, gain_ref),
                (lengths_hbm, lengths_ref),
                (lambda_hbm, lambda_ref),
                (head_gain_hbm, head_gain_ref),
            )
        )
    ]
    for copy in small:
        copy.start()
    large = [
        pltpu.make_async_copy(source, target, large_sem.at[i])
        for i, (source, target) in enumerate(
            (
                (query_hbm, weights_ref.at[0]),
                (key_hbm, weights_ref.at[1]),
                (value_hbm, weights_ref.at[2]),
                (keys_hbm, keys_ref),
                (values_hbm, values_ref),
                (out_hbm, out_ref),
            )
        )
    ]
    for i in (0, 1, 2, 3):
        large[i].start()
    for copy in small:
        copy.wait()
    large[4].start()
    large[5].start()
    normed = norm_rows(tokens_ref[...], gain_ref[...]).astype(bf16)
    spread = (
        lax.broadcasted_iota(jnp.int32, (lanes, heads * lanes), 1) // heads
        == lax.broadcasted_iota(jnp.int32, (lanes, heads * lanes), 0)
    ).astype(bf16)
    lane_head = lax.broadcasted_iota(jnp.int32, (seqs, heads * lanes), 1) % heads
    for block in range(model_width // lanes):
        part = jnp.dot(
            normed[:, block * lanes : (block + 1) * lanes], spread, preferred_element_type=f32
        )
        columns = slice(block * heads * lanes, (block + 1) * heads * lanes)
        for h in range(heads):
            wide_ref[h * seqs : (h + 1) * seqs, columns] = jnp.where(
                lane_head == h, part, 0.0
            ).astype(bf16)

    row_ids = lax.broadcasted_iota(jnp.int32, (rows, heads * seqs), 0)
    column_ids = lax.broadcasted_iota(jnp.int32, (rows, heads * seqs), 1)
    placing = (
        (column_ids % seqs == row_ids // group_rows)
        & (column_ids // seqs == (row_ids % group_rows) // 2 % heads)
    ).astype(bf16)

    def project(i):
        large[i].wait()
        product = jnp.dot(wide_ref[...], weights_ref[i], preferred_element_type=f32)
        return jnp.dot(placing, product.astype(bf16), preferred_element_type=f32)

    place = lax.broadcasted_iota(jnp.int32, (rows, head_width), 0) % group_rows
    lane = lax.broadcasted_iota(jnp.int32, (rows, head_width), 1)
    own_half = ((lane < head_width // 2) == (place % 2 == 0)) & (place < 2 * heads)
    queries = jnp.where(own_half, project(0), 0.0) * (head_width // 2) ** (-0.5)
    query_ref[...] = queries
    own_scores = jnp.sum(queries * project(1), axis=-1, keepdims=True)
    value_new = project(2)

    group = lax.broadcasted_iota(jnp.int32, (group_rows, positions), 0)
    spot = lax.broadcasted_iota(jnp.int32, (group_rows, positions), 1)
    own_head = spot % heads == group // 2 % heads
    spot = jnp.where(own_head, spot, positions)

    def folded(source, combine):
        parts = [source[:, i : i + lanes] for i in range(0, positions, lanes)]
        while len(parts) > 1:
            parts = [combine(a, b) for a, b in zip(parts[::2], parts[1::2])]
        return parts[0]

    large[3].wait()
    for s in range(seqs):
        at = slice(s * group_rows, (s + 1) * group_rows)
        scores = lax.dot_general(
            query_ref[at, :].astype(bf16),
            keys_ref[s],
            (((1,), (1,)), ((), ())),
            preferred_element_type=f32,
        )
        scores = jnp.where(spot < lengths_ref[s] * heads, scores, -jnp.inf)
        scores_ref[at, :] = scores
        peak_ref[at, :] = folded(scores, jnp.maximum)

    peak = jnp.maximum(jnp.max(peak_ref[...], axis=-1, keepdims=True), own_scores)
    peak_ref[...] = jnp.broadcast_to(peak, peak_ref.shape)
    for s in range(seqs):
        at = slice(s * group_rows, (s + 1) * group_rows)
        shifted = jnp.exp(scores_ref[at, :] - peak_ref[at, 0:1])
        scores_ref[at, :] = shifted
        total_ref[at, :] = folded(shifted, jnp.add)

    own_weight = jnp.exp(own_scores - peak)
    denominator = jnp.sum(total_ref[...], axis=-1, keepdims=True) + own_weight
    row = lax.broadcasted_iota(jnp.int32, (rows, 1), 0) % group_rows
    factor = jnp.ones((rows, 1), f32)
    for h in range(heads):
        factor = jnp.where(row == 2 * h + 1, -lambda_ref[h], factor)
    factor = factor / denominator
    peak_ref[...] = jnp.broadcast_to(factor, peak_ref.shape)
    total_ref[...] = jnp.broadcast_to(own_weight * factor, peak_ref.shape)
    query_ref[...] = value_new

    def mixed(source):
        return (source + pltpu.roll(source, group_rows - 1, 0)).astype(bf16)

    large[4].wait()
    for s in range(seqs):
        at = slice(s * group_rows, (s + 1) * group_rows)
        weights = mixed(scores_ref[at, :] * peak_ref[at, 0:1])
        own = mixed(total_ref[at, :]).astype(f32)
        heads_ref[at, :] = (
            jnp.dot(weights, values_ref[s], preferred_element_type=f32)
            + own * query_ref[at, :]
        )

    heads_out = heads_ref[...]
    normed_heads = (
        heads_out
        * lax.rsqrt(jnp.mean(heads_out * heads_out, axis=-1, keepdims=True) + epsilon)
        * head_gain_ref[...]
        * branch_scale
    ).astype(bf16)
    picked = []
    taker = lax.broadcasted_iota(jnp.int32, (seqs, rows), 0) * group_rows
    giver = lax.broadcasted_iota(jnp.int32, (seqs, rows), 1)
    for h in range(heads):
        chosen = (giver == taker + 2 * h).astype(bf16)
        picked.append(jnp.dot(chosen, normed_heads, preferred_element_type=f32).astype(bf16))
    joined = jnp.concatenate(picked, axis=1) if heads > 1 else picked[0]
    large[5].wait()
    core = lax.axis_index("core")
    for y in range(rows_y):
        for target, which in ((sent_ref, 1 - core), (kept_ref, core)):
            columns = pl.ds(pl.multiple_of((2 * y + which) * width, width), width)
            target[y] = jnp.dot(
                joined, out_ref[:, columns], preferred_element_type=f32
            ).astype(bf16)


def attend(
    tokens,
    lengths,
    key_cache,
    value_cache,
    attn_gain,
    w_query,
    w_key,
    w_value,
    mix_lambda,
    head_gain,
    w_out,
    rows_y,
):
    seqs, model_width = tokens.shape
    cache_len, heads, head_width = key_cache.shape[1:]
    positions = cache_len * heads
    rows = seqs * group_rows
    width = model_width // (2 * rows_y)
    bf16, f32 = jnp.bfloat16, jnp.float32
    vmem = pl.BlockSpec(memory_space=pltpu.VMEM)
    hbm = pl.BlockSpec(memory_space=pltpu.HBM)
    out = jax.ShapeDtypeStruct((rows_y, seqs, width), bf16)
    return pl.pallas_call(
        attention_kernel,
        out_shape=(out, out),
        in_specs=[hbm] * 11,
        out_specs=(vmem, vmem),
        scratch_shapes=[
            pltpu.SMEM((seqs,), jnp.int32),
            pltpu.SMEM((heads,), f32),
            pltpu.VMEM((seqs, model_width), bf16),
            pltpu.VMEM((1, model_width), f32),
            pltpu.VMEM((1, head_width), f32),
            pltpu.VMEM((3, model_width * heads, head_width), bf16),
            pltpu.VMEM((seqs, positions, head_width), bf16),
            pltpu.VMEM((seqs, positions, head_width), bf16),
            pltpu.VMEM((heads * head_width, model_width), bf16),
            pltpu.VMEM((heads * seqs, heads * model_width), bf16),
            pltpu.VMEM((rows, head_width), f32),
            pltpu.VMEM((rows, positions), f32),
            pltpu.VMEM((rows, 128), f32),
            pltpu.VMEM((rows, 128), f32),
            pltpu.VMEM((rows, head_width), f32),
            pltpu.SemaphoreType.DMA((5,)),
            pltpu.SemaphoreType.DMA((6,)),
        ],
        compiler_params=pltpu.CompilerParams(vmem_limit_bytes=attention_vmem),
        cost_estimate=pl.CostEstimate(
            flops=attention_flops, bytes_accessed=4 * key_cache.size, transcendentals=0
        ),
        name="attention",
    )(
        lengths,
        mix_lambda,
        tokens,
        attn_gain.reshape(1, model_width),
        head_gain.reshape(1, head_width),
        w_query.reshape(model_width * heads, head_width),
        w_key.reshape(model_width * heads, head_width),
        w_value.reshape(model_width * heads, head_width),
        key_cache.reshape(seqs, positions, head_width),
        value_cache.reshape(seqs, positions, head_width),
        w_out.reshape(heads * head_width, model_width),
    )


attention_vmem = 63 * 1024 * 1024
attention_flops = 4 * 10**9


def expert_kernel(
    own_ref,
    other_ref,
    gain_ref,
    gate_hbm,
    up_hbm,
    down_hbm,
    kept_ref,
    sent_ref,
    gate_ref,
    up_ref,
    down_ref,
    weight_sem,
):
    copies = [
        pltpu.make_async_copy(source, target, weight_sem.at[i])
        for i, (source, target) in enumerate(
            ((gate_hbm, gate_ref), (up_hbm, up_ref), (down_hbm, down_ref))
        )
    ]
    for copy in copies:
        copy.start()
    rows_y, _, width = kept_ref.shape
    model_width = gain_ref.shape[1]
    f32, bf16 = jnp.float32, jnp.bfloat16
    core = lax.axis_index("core")
    sides = ((own_ref, core), (other_ref, 1 - core))

    def columns(y, which):
        return pl.ds(pl.multiple_of((2 * y + which) * width, width), width)

    total = 0.0
    for source, _ in sides:
        wide = source[...].astype(f32)
        total = total + jnp.sum(wide * wide, axis=-1, keepdims=True)
    scale = lax.rsqrt(total / model_width + epsilon)
    normed = []
    for source, which in sides:
        for y in range(rows_y):
            at = columns(y, which)
            wide = source[:, y * width : (y + 1) * width].astype(f32)
            normed.append(((wide * scale * gain_ref[:, at]).astype(bf16), at))
    products = []
    for copy, weight in zip(copies, (gate_ref, up_ref)):
        copy.wait()
        product = 0.0
        for part, at in normed:
            product = product + jnp.dot(part, weight[at, :], preferred_element_type=f32)
        products.append(product)
    gate_value, up_value = products
    gate_value = jnp.minimum(gate_value, clamp_limit)
    up_value = jnp.clip(up_value, -clamp_limit, clamp_limit)
    activated = ((up_value + 1.0) * gate_value * jax.nn.sigmoid(sigmoid_slope * gate_value)).astype(
        bf16
    )
    copies[2].wait()
    for target, which in ((sent_ref, 1 - core), (kept_ref, core)):
        for y in range(rows_y):
            target[y] = jnp.dot(
                activated, down_ref[:, columns(y, which)], preferred_element_type=f32
            ).astype(bf16)


def apply_expert(own, other, ffn_gain, w_gate, w_up, w_down, rows_y):
    rows, half = own.shape
    model_width, hidden = w_gate.shape
    out = jax.ShapeDtypeStruct((rows_y, rows, half // rows_y), jnp.bfloat16)
    vmem = pl.BlockSpec(memory_space=pltpu.VMEM)
    return pl.pallas_call(
        expert_kernel,
        out_shape=(out, out),
        in_specs=[vmem] * 3 + [pl.BlockSpec(memory_space=pltpu.HBM)] * 3,
        out_specs=(vmem, vmem),
        scratch_shapes=[
            pltpu.VMEM((model_width, hidden), jnp.bfloat16),
            pltpu.VMEM((model_width, hidden), jnp.bfloat16),
            pltpu.VMEM((hidden, model_width), jnp.bfloat16),
            pltpu.SemaphoreType.DMA((3,)),
        ],
        compiler_params=pltpu.CompilerParams(vmem_limit_bytes=expert_vmem),
        cost_estimate=pl.CostEstimate(
            flops=6 * rows * model_width * hidden,
            bytes_accessed=6 * model_width * hidden,
            transcendentals=rows * hidden,
        ),
        name="expert",
    )(own, other, ffn_gain.reshape(1, model_width), w_gate, w_up, w_down)


expert_vmem = 53 * 1024 * 1024


def per_device(
    tokens,
    lengths,
    key_cache,
    value_cache,
    attn_gain,
    w_query,
    w_key,
    w_value,
    mix_lambda,
    head_gain,
    w_out,
    ffn_gain,
    w_gate,
    w_up,
    w_down,
    routes,
    route_weights,
):
    seq_dev, model_width = tokens.shape
    own_core = lax.axis_index("core")
    rows_y = lax.axis_size("y")
    width = model_width // (2 * rows_y)
    experts = lax.axis_size("ep")
    top_count = routes.shape[1]
    capacity = min(seq_dev, 2 * seq_dev * top_count // experts)

    def halves_of(source):
        blocks = source.reshape(source.shape[0], rows_y, 2, width)
        kept = lax.dynamic_index_in_dim(blocks, own_core, 2, keepdims=False)
        sent = lax.dynamic_index_in_dim(blocks, 1 - own_core, 2, keepdims=False)
        return kept, sent

    def swap_cores(source):
        return lax.ppermute(source, "core", [(0, 1), (1, 0)])

    def add_swapped(kept, sent):
        arrived = swap_cores(sent)
        return (kept.astype(jnp.float32) + arrived.astype(jnp.float32)).astype(jnp.bfloat16)

    kept, sent = attend(
        tokens,
        lengths,
        key_cache,
        value_cache,
        attn_gain,
        w_query,
        w_key,
        w_value,
        mix_lambda,
        head_gain,
        w_out,
        rows_y,
    )
    pair = add_swapped(kept, sent)
    if rows_y == 2:
        other = lax.ppermute(pair, "y", [(0, 1), (1, 0)])
        attention = pair.astype(jnp.float32) + other.astype(jnp.float32)
    else:
        attention = jnp.sum(lax.all_gather(pair, "y").astype(jnp.float32), axis=0)
    attention = attention.transpose(1, 0, 2)
    own_tokens, _ = halves_of(tokens)
    residual = (own_tokens.astype(jnp.float32) + attention).astype(jnp.bfloat16)
    half_width_all = rows_y * width
    flat_residual = residual.reshape(seq_dev, half_width_all)
    if capacity < seq_dev:
        entries = routes.reshape(-1)
        onehot = (entries[:, None] == lax.iota(jnp.int32, experts)[None, :]).astype(jnp.int32)
        entry_slot = jnp.sum((jnp.cumsum(onehot, axis=0) - onehot) * onehot, axis=-1)
        target = (entries * capacity + entry_slot).reshape(seq_dev, top_count)
        slot_ids = lax.iota(jnp.int32, experts * capacity)
        chosen = (target[..., None] == slot_ids[None, None, :]).astype(jnp.float32)
        placing = jnp.sum(chosen, axis=1).astype(jnp.bfloat16)
        outgoing = lax.dot_general(
            placing, flat_residual, (((0,), (0,)), ((), ())), preferred_element_type=jnp.float32
        ).astype(jnp.bfloat16)
        outgoing = outgoing.reshape(experts, capacity, half_width_all)
    else:
        outgoing = jnp.broadcast_to(flat_residual[None], (experts, seq_dev, half_width_all))
    arrived = lax.all_to_all(outgoing, "ep", split_axis=0, concat_axis=0, tiled=True)
    own_half = arrived.reshape(experts * capacity, half_width_all)
    kept, sent = apply_expert(
        own_half, swap_cores(own_half), ffn_gain, w_gate[0], w_up[0], w_down[0], rows_y
    )
    pieces = add_swapped(kept, sent).reshape(rows_y * experts, capacity, width)
    returned = lax.all_to_all(pieces, ("y", "ep"), split_axis=0, concat_axis=0, tiled=True)
    returned = returned.reshape(rows_y, experts, capacity, width).astype(jnp.float32)
    expert_out = jnp.sum(returned, axis=0).astype(jnp.bfloat16).astype(jnp.float32)
    if capacity < seq_dev:
        combine = jnp.sum(route_weights[..., None] * chosen, axis=1)
        expert_sum = jnp.dot(
            combine, expert_out.reshape(experts * capacity, width), precision=lax.Precision.HIGHEST
        )
    else:
        named = routes[..., None] == lax.iota(jnp.int32, experts)[None, None, :]
        weights = jnp.sum(jnp.where(named, route_weights[..., None], 0.0), axis=1)
        expert_sum = jnp.sum(weights.T[:, :, None] * expert_out, axis=0)
    own_columns = lax.dynamic_index_in_dim(residual, lax.axis_index("y"), 1, keepdims=False)
    return (own_columns.astype(jnp.float32) + expert_sum).astype(jnp.bfloat16)


def solution(mesh):
    experts, shards = mesh.shape["ep"], mesh.shape["tp"]
    split = jax.sharding.Mesh(mesh.devices.reshape(experts, shards // 2, 2), ("ep", "y", "core"))
    tp = ("y", "core")
    placed = (
        P("ep", None),
        P("ep"),
        P("ep", None, tp, None),
        P("ep", None, tp, None),
        P(),
        P(None, tp, None),
        P(None, tp, None),
        P(None, tp, None),
        P(tp),
        P(),
        P(tp, None, None),
        P(),
        P("ep", None, tp),
        P("ep", None, tp),
        P("ep", tp, None),
        P("ep", None),
        P("ep", None),
    )
    return jax.shard_map(
        per_device, mesh=split, in_specs=placed, out_specs=P("ep", tp), check_vma=False
    )
```
